32 devices in a mesh: sp: 8 (over z, y), tp: 4 (over x, core).
Axes of the slice: x: 2, y: 2, z: 4, core: 2. Of those that a mesh axis runs over, the one named last changes fastest.
Arguments:
- tokens: bfloat16 [4096, 2048], P('sp'), may hold values from -6 to 6
- norm_gain: bfloat16 [2048], replicated, may hold values from 0.099609375 to 1.8984375
- w_conv_value: bfloat16 [2048, 2048], P('sp', 'tp'), may hold values from -0.125 to 0.125
- w_conv_gate: bfloat16 [2048, 2048], P('sp', 'tp'), may hold values from -0.125 to 0.125
- w_query: bfloat16 [2048, 2048], P('sp', 'tp'), may hold values from -0.125 to 0.125
- w_key: bfloat16 [2048, 512], P('sp', 'tp'), may hold values from -0.125 to 0.125
- w_value: bfloat16 [2048, 512], P('sp', 'tp'), may hold values from -0.125 to 0.125
- conv_taps: float32 [31, 2048], P(None, 'tp'), as said below
- ln_gain: float32 [2048], P('tp'), may hold values from 0.1 to 1.9
- sinks: float32 [32], P('tp'), may hold values from 3 to 6
- out_conv: bfloat16 [2048, 2048], P('tp', 'sp'), may hold values from -0.125 to 0.125
- out_attn: bfloat16 [2048, 2048], P('tp', 'sp'), may hold values from -0.5 to 0.5
Outputs:
- mixed: bfloat16 [4096, 2048], P(('sp', 'tp'))
- log_sums: float32 [32, 4096], P('tp', 'sp')
The draws below stay inside these ranges and needn't reach their ends.
Inputs may be any that keep to these rules, and one draw needn't show every extreme that they name: `conv_taps`: each tap lies within 30 / sqrt(31) in magnitude.
All inputs are finite; a program needn't handle non-finite values.
Results may differ from the reference program's by a relative error of at most 0.017.
Values may be sent and summed in bfloat16 or wider, within the bound.
A program may use at most 64 MiB of HBM per device.

```python
import jax
import jax.numpy as jnp
from jax import lax

D = 2048
CONV_CH = 2048
HEADS = 32
KV_HEADS = 8
HEAD_DIM = 64
CONV_K = 31
WINDOW = 128
TOKENS = 4096
SPLITS = 4


def draw_conv_taps(key, part):
    channel = jnp.arange(CONV_CH, dtype=jnp.float32)
    samples = jax.random.truncated_normal(key, -3.0, 3.0, (CONV_K, CONV_CH), jnp.float32)
    scales = 10.0 ** (channel / CONV_CH)
    return samples * scales[None, :] * CONV_K ** (-0.5)


def steps_of(own_key, extent, split, low, top_value):
    def one(position, shards_of):
        steps = jax.random.uniform(jax.random.fold_in(jax.random.fold_in(own_key, 6), position), (shards_of,), jnp.float32, low / len(split), top_value / len(split))
        return jnp.repeat(jnp.exp(steps), extent[position] // shards_of).reshape((-1,) + (1,) * (len(extent) - position - 1))

    gain = one(*split[0])
    for cut in split[1:]:
        gain = gain * one(*cut)
    return gain


def noise(rng, shape, spread, most, pieces=(), held_as=jnp.bfloat16):
    array = spread * jax.random.normal(rng, shape, jnp.float32)
    if pieces:
        array = array * steps_of(rng, shape, pieces, -0.22, 0.18)
    return jnp.clip(array, -most, most).astype(held_as)


def setup_inputs(seed: int = 0) -> dict:
    arg_keys = jax.random.split(jax.random.key(seed), 13)
    tokens = noise(arg_keys[0], (TOKENS, D), 1.0, 6.0, ((0, 8),))
    norm_gain = jnp.clip(1.0 + 0.18 * jax.random.normal(arg_keys[1], (D,), jnp.float32), 0.099609375, 1.8984375).astype(jnp.bfloat16)
    w_conv_value = noise(arg_keys[2], (D, CONV_CH), D ** -0.5, 0.125, ((0, 8), (1, 4)))
    w_conv_gate = noise(arg_keys[3], (D, CONV_CH), D ** -0.5, 0.125, ((0, 8), (1, 4)))
    w_query = noise(arg_keys[4], (D, HEADS * HEAD_DIM), D ** -0.5, 0.125, ((0, 8), (1, 4)))
    w_key = noise(arg_keys[5], (D, KV_HEADS * HEAD_DIM), D ** -0.5, 0.125, ((0, 8), (1, 4)))
    w_value = noise(arg_keys[6], (D, KV_HEADS * HEAD_DIM), D ** -0.5, 0.125, ((0, 8), (1, 4)))
    conv_taps = draw_conv_taps(jax.random.fold_in(arg_keys[12], 71), 0)
    ln_gain = jnp.clip(1.0 + 0.18 * jax.random.normal(arg_keys[8], (CONV_CH,), jnp.float32), 0.1, 1.9)
    sinks = jnp.clip(3.0 + 3.0 * jax.random.uniform(arg_keys[9], (HEADS,), jnp.float32) ** steps_of(arg_keys[9], (HEADS,), ((0, 4),), -0.2, 0.2), 3.0, 6.0)
    out_conv = noise(arg_keys[10], (CONV_CH, D), CONV_CH ** -0.5, 0.125, ((0, 4), (1, 8)))
    out_attn = noise(arg_keys[11], (HEADS * HEAD_DIM, D), (HEADS * HEAD_DIM // 16) ** -0.5, 0.5, ((0, 4), (1, 8)))
    return dict(tokens=tokens, norm_gain=norm_gain, w_conv_value=w_conv_value, w_conv_gate=w_conv_gate, w_query=w_query, w_key=w_key, w_value=w_value, conv_taps=conv_taps, ln_gain=ln_gain, sinks=sinks, out_conv=out_conv, out_attn=out_attn)


NORM_EPS = 1e-06
CHANNEL_EPS = 1e-05
ROPE_BASE = 10000.0

def rotate(heads, positions):
    half_dim = heads.shape[-1] // 2
    inverse = ROPE_BASE ** (-jnp.arange(half_dim, dtype=jnp.float32) / half_dim)
    angles = positions.astype(jnp.float32)[:, None] * inverse[None, :]
    cosine = jnp.cos(angles)[:, None, :]
    sine = jnp.sin(angles)[:, None, :]
    as_float = heads.astype(jnp.float32)
    front_part = as_float[..., :half_dim]
    back_part = as_float[..., half_dim:]
    return jnp.concatenate([front_part * cosine - back_part * sine, back_part * cosine + front_part * sine], axis=-1)

def reference(tokens, norm_gain, w_conv_value, w_conv_gate, w_query, w_key, w_value, conv_taps, ln_gain, sinks, out_conv, out_attn):
    as_float = tokens.astype(jnp.float32)
    normed = (as_float * lax.rsqrt(lax.optimization_barrier(jnp.mean(as_float * as_float, axis=-1, keepdims=True)) + NORM_EPS) * norm_gain.astype(jnp.float32)).astype(jnp.bfloat16)

    def project(weight):
        return jnp.dot(normed, weight, preferred_element_type=jnp.float32).astype(jnp.bfloat16)
    conv_value = project(w_conv_value)
    conv_gate = project(w_conv_gate)
    query_raw = project(w_query)
    key_raw = project(w_key)
    value_rows = project(w_value)
    glu = (conv_value.astype(jnp.float32) * jax.nn.sigmoid(conv_gate.astype(jnp.float32))).astype(jnp.bfloat16)
    padded = jnp.concatenate([jnp.zeros((CONV_K - 1, CONV_CH), jnp.float32), glu.astype(jnp.float32)], axis=0)
    conv_out = jnp.zeros((TOKENS, CONV_CH), jnp.float32)
    for tap in range(CONV_K):
        conv_out = conv_out + conv_taps[tap].astype(jnp.float32)[None, :] * padded[tap:tap + TOKENS]
    mean = lax.optimization_barrier(jnp.mean(conv_out, axis=-1, keepdims=True))
    var = lax.optimization_barrier(jnp.mean(conv_out * conv_out, axis=-1, keepdims=True)) - mean * mean
    conv_branch = jax.nn.silu((conv_out - mean) * lax.rsqrt(var + CHANNEL_EPS) * ln_gain.astype(jnp.float32)[None, :]).astype(jnp.bfloat16)
    positions = jnp.arange(TOKENS, dtype=jnp.int32)
    query = rotate(query_raw.reshape(TOKENS, HEADS, HEAD_DIM), positions).astype(jnp.bfloat16)
    key = rotate(key_raw.reshape(TOKENS, KV_HEADS, HEAD_DIM), positions).astype(jnp.bfloat16)
    values = value_rows.reshape(TOKENS, KV_HEADS, HEAD_DIM)
    group = HEADS // KV_HEADS
    blocks = TOKENS // WINDOW
    q_blocks = query.reshape(blocks, WINDOW, KV_HEADS, group, HEAD_DIM).astype(jnp.float32)
    leading = jnp.zeros((WINDOW, KV_HEADS, HEAD_DIM), jnp.bfloat16)
    key_blocks = jnp.concatenate([leading, key], axis=0).reshape(blocks + 1, WINDOW, KV_HEADS, HEAD_DIM)
    value_blocks = jnp.concatenate([leading, values], axis=0).reshape(blocks + 1, WINDOW, KV_HEADS, HEAD_DIM)
    key_window = jnp.concatenate([key_blocks[:-1], key_blocks[1:]], axis=1).astype(jnp.float32)
    value_window = jnp.concatenate([value_blocks[:-1], value_blocks[1:]], axis=1).astype(jnp.float32)
    scores = jnp.einsum('nqhgd,nkhd->nhgqk', q_blocks, key_window) * HEAD_DIM ** (-0.5)
    query_index = jnp.arange(WINDOW)[:, None] + WINDOW
    key_index = jnp.arange(2 * WINDOW)[None, :]
    band = (key_index <= query_index) & (query_index - key_index < WINDOW)
    block_index = jnp.arange(blocks)[:, None, None]
    allowed = band[None] & (block_index * WINDOW + key_index[None] - WINDOW >= 0)
    allowed = allowed[:, None, None]
    totals = lax.optimization_barrier(jnp.sum(jnp.where(allowed, jnp.exp(scores), 0.0), axis=-1))
    totals = totals + jnp.exp(sinks.astype(jnp.float32)).reshape(1, KV_HEADS, group, 1)
    log_total = jnp.log(totals)
    weights = jnp.where(allowed, jnp.exp(scores - log_total[..., None]), 0.0).astype(jnp.bfloat16)
    attended = jnp.einsum('nhgqk,nkhd->nqhgd', weights.astype(jnp.float32), value_window)
    attn_branch = attended.astype(jnp.bfloat16).reshape(TOKENS, HEADS * HEAD_DIM)
    log_sums = log_total.transpose(1, 2, 0, 3).reshape(HEADS, TOKENS)
    conv_width = CONV_CH // SPLITS
    attn_width = HEADS * HEAD_DIM // SPLITS
    mixed = jnp.zeros((TOKENS, D), jnp.float32)
    for index in range(SPLITS):
        part_sum = jnp.dot(conv_branch[:, index * conv_width:(index + 1) * conv_width], out_conv[index * conv_width:(index + 1) * conv_width], preferred_element_type=jnp.float32)
        part_sum = part_sum + jnp.dot(attn_branch[:, index * attn_width:(index + 1) * attn_width], out_attn[index * attn_width:(index + 1) * attn_width], preferred_element_type=jnp.float32)
        rounded = lax.optimization_barrier(part_sum.astype(jnp.bfloat16))
        mixed = mixed + rounded.astype(jnp.float32)
    return (mixed.astype(jnp.bfloat16), log_sums)
```

```python
import functools

import jax
import jax.numpy as jnp
from jax import lax
from jax.experimental import pallas as pl
from jax.experimental.pallas import tpu as pltpu
from jax.sharding import PartitionSpec as P

CONV_CH = 2048
HEADS = 32
KV_HEADS = 8
HEAD_DIM = 64
WINDOW = 128


NORM_EPS = 1e-06
CHANNEL_EPS = 1e-05
ROPE_BASE = 10000.0


def shifted(value, axis, steps):
    count = lax.axis_size(axis)
    initial, last = (max(0, -steps), min(count, count - steps))
    return lax.ppermute(value, axis, [(source, source + steps) for source in range(initial, last)])


def rotate(heads, positions):
    half_dim = heads.shape[-1] // 2
    inverse = ROPE_BASE ** (-jnp.arange(half_dim, dtype=jnp.float32) / half_dim)
    angles = positions.astype(jnp.float32)[:, None] * inverse[None, :]
    cosine = jnp.cos(angles)[:, None, :]
    sine = jnp.sin(angles)[:, None, :]
    as_float = heads.astype(jnp.float32)
    front_part = as_float[..., :half_dim]
    back_part = as_float[..., half_dim:]
    return jnp.concatenate(
        [front_part * cosine - back_part * sine, back_part * cosine + front_part * sine], axis=-1
    )


def ring_place(index, count):
    half = count // 2
    index = lax.rem(index + 2 * count, count)
    return jnp.where(index < half, 2 * index, 2 * (count - 1 - index) + 1)


class Ring:
    def __init__(self, count, phases, send_sem, recv_sem):
        self.count, self.phases = count, phases
        self.send_sem, self.recv_sem = send_sem, recv_sem
        me = lax.axis_index("sp")
        half = count // 2
        spot = jnp.where(lax.rem(me, 2) == 0, me // 2, count - 1 - me // 2)
        self.spot = spot
        self.peers = (ring_place(spot + 1, count), ring_place(spot - 1, count))

    def owner(self, way, step):
        return ring_place(self.spot - step if way == 0 else self.spot + step, self.count)

    def copy(self, phase, way, piece, step):
        own, place = self.phases[phase][way][piece]
        target = place(self.owner(way, step))
        number = sum(len(p[0]) for p in self.phases[:phase]) + piece
        return pltpu.make_async_remote_copy(
            src_ref=own if step == 0 else target,
            dst_ref=target,
            send_sem=self.send_sem.at[way, number, step],
            recv_sem=self.recv_sem.at[way, number, step],
            device_id={"sp": self.peers[way]},
            device_id_type=pl.DeviceIdType.MESH,
        )

    def arrived(self, phase, way, piece, step):
        own, place = self.phases[phase][way][piece]
        target = place(self.owner(way, step + 1))
        number = sum(len(p[0]) for p in self.phases[:phase]) + piece
        pltpu.make_async_remote_copy(
            src_ref=target,
            dst_ref=target,
            send_sem=self.send_sem.at[way, number, step],
            recv_sem=self.recv_sem.at[way, number, step],
            device_id={"sp": self.peers[way]},
            device_id_type=pl.DeviceIdType.MESH,
        ).wait_recv()

    def begin(self, phase):
        for piece in range(len(self.phases[phase][0])):
            for way in range(2):
                self.copy(phase, way, piece, 0).start()

    def advance(self, phase, step):
        for piece in range(len(self.phases[phase][0])):
            for way in range(2):
                self.arrived(phase, way, piece, step)
                if step + 1 < self.count - 1:
                    self.copy(phase, way, piece, step + 1).start()

    def drain(self):
        for phase in range(len(self.phases)):
            for piece in range(len(self.phases[phase][0])):
                for way in range(2):
                    for step in range(self.count - 1):
                        self.copy(phase, way, piece, step).wait_send()


def run_phase(ring, phase, work):
    steps = ring.count - 1
    done = 0
    for step in range(steps):
        upto = (step + 1) * len(work) // steps
        for item in work[done:upto]:
            item()
        done = upto
        ring.advance(phase, step)
        if step == steps - 2 and phase + 1 < len(ring.phases):
            ring.begin(phase + 1)


def gather_kernel(
    count,
    tokens,
    norm_gain,
    w_conv_value,
    w_conv_gate,
    w_query,
    w_key,
    w_value,
    out_conv,
    out_attn,
    glu_out,
    query_out,
    key_out,
    value_out,
    full_conv,
    full_attn,
    normed,
    full_cv,
    full_cg,
    full_q,
    full_k,
    full_v,
    send_sem,
    recv_sem,
    own_sem,
):
    me = lax.axis_index("sp")
    depth, wide = w_query.shape
    narrow = w_key.shape[1]
    long, cols = out_conv.shape
    rows = tokens.shape[0]

    def by_rows(own, full, low, high):
        return (
            own.at[:, pl.ds(low, high - low)],
            lambda who: full.at[
                pl.ds(pl.multiple_of(who * depth, depth), depth), pl.ds(low, high - low)
            ],
        )

    def by_cols(own, full, low, high):
        return (
            own.at[pl.ds(low, high - low)],
            lambda who: full.at[
                pl.ds(low, high - low), pl.ds(pl.multiple_of(who * cols, cols), cols)
            ],
        )

    quarter, middle = wide // 4, wide // 2
    phases = (
        (
            [by_rows(w_query, full_q, i * quarter, (i + 1) * quarter) for i in range(3)],
            [
                by_rows(w_query, full_q, 3 * quarter, wide),
                by_rows(w_key, full_k, 0, narrow),
                by_rows(w_value, full_v, 0, narrow),
            ],
        ),
        (
            [by_rows(w_conv_value, full_cv, i * middle, (i + 1) * middle) for i in range(2)],
            [by_rows(w_conv_gate, full_cg, i * middle, (i + 1) * middle) for i in range(2)],
        ),
        (
            [by_cols(out_conv, full_conv, i * long // 2, (i + 1) * long // 2) for i in range(2)],
            [by_cols(out_attn, full_attn, i * long // 2, (i + 1) * long // 2) for i in range(2)],
        ),
    )
    ring = Ring(count, phases, send_sem, recv_sem)
    barrier = pltpu.get_barrier_semaphore()
    for peer in ring.peers:
        pl.semaphore_signal(
            barrier, inc=1, device_id={"sp": peer}, device_id_type=pl.DeviceIdType.MESH
        )
    pl.semaphore_wait(barrier, 2)
    ring.begin(0)

    mine = pl.ds(pl.multiple_of(me * depth, depth), depth)
    my_cols = pl.ds(pl.multiple_of(me * cols, cols), cols)
    local = [
        pltpu.make_async_copy(own, place, own_sem.at[i])
        for i, (own, place) in enumerate(
            (
                (w_conv_value, full_cv.at[mine]),
                (w_conv_gate, full_cg.at[mine]),
                (w_query, full_q.at[mine]),
                (w_key, full_k.at[mine]),
                (w_value, full_v.at[mine]),
                (out_conv, full_conv.at[:, my_cols]),
                (out_attn, full_attn.at[:, my_cols]),
            )
        )
    ]
    for item in local:
        item.start()

    def norm(part):
        take = pl.ds(part * 64, 64)
        x = tokens[take, :].astype(jnp.float32)
        scale = lax.rsqrt(jnp.mean(x * x, axis=-1, keepdims=True) + NORM_EPS)
        normed[take, :] = (x * scale * norm_gain[...].astype(jnp.float32)).astype(jnp.bfloat16)

    def product(take, full):
        return jnp.dot(normed[take, :], full[...], preferred_element_type=jnp.float32).astype(
            jnp.bfloat16
        )

    def attention_side(part):
        take = pl.ds(part * 128, 128)
        query_out[take, :] = product(take, full_q)
        key_out[take, :] = product(take, full_k)
        value_out[take, :] = product(take, full_v)

    def conv_side(part):
        take = pl.ds(part * 128, 128)
        value = product(take, full_cv).astype(jnp.float32)
        gate = product(take, full_cg).astype(jnp.float32)
        glu_out[take, :] = (value * jax.nn.sigmoid(gate)).astype(jnp.bfloat16)

    run_phase(ring, 0, [functools.partial(norm, i) for i in range(rows // 64)])
    for item in local:
        item.wait()
    run_phase(ring, 1, [functools.partial(attention_side, i) for i in range(rows // 128)])
    run_phase(ring, 2, [functools.partial(conv_side, i) for i in range(rows // 128)])
    ring.drain()


def fits(count, shape_in, shape_out, rows):
    tiled = shape_in[0] % 128 == 0 and shape_in[1] % 512 == 0 and shape_out[1] % 128 == 0
    return tiled and rows % 128 == 0 and count % 2 == 0 and count > 3


def gathered(
    tokens, norm_gain, w_conv_value, w_conv_gate, w_query, w_key, w_value, out_conv, out_attn
):
    count = lax.axis_size("sp")
    rows, width = tokens.shape
    wide, narrow = w_query.shape[1], w_key.shape[1]
    long = out_conv.shape[0]
    vmem = pl.BlockSpec(memory_space=pltpu.VMEM)
    shape = lambda *dims: jax.ShapeDtypeStruct(dims, jnp.bfloat16)
    scratch = lambda *dims: pltpu.VMEM(dims, jnp.bfloat16)
    pieces = 7
    return pl.pallas_call(
        functools.partial(gather_kernel, count),
        out_shape=(
            shape(rows, w_conv_value.shape[1]),
            shape(rows, wide),
            shape(rows, narrow),
            shape(rows, narrow),
            shape(long, count * out_conv.shape[1]),
            shape(out_attn.shape[0], count * out_attn.shape[1]),
        ),
        in_specs=[vmem] * 9,
        out_specs=(vmem,) * 6,
        scratch_shapes=[
            scratch(rows, width),
            scratch(width, w_conv_value.shape[1]),
            scratch(width, w_conv_gate.shape[1]),
            scratch(width, wide),
            scratch(width, narrow),
            scratch(width, narrow),
            pltpu.SemaphoreType.DMA((2, pieces, count - 1)),
            pltpu.SemaphoreType.DMA((2, pieces, count - 1)),
            pltpu.SemaphoreType.DMA((7,)),
        ],
        compiler_params=pltpu.CompilerParams(collective_id=0, has_side_effects=True),
        name="gather_project",
    )(
        tokens,
        norm_gain.reshape(1, width),
        w_conv_value,
        w_conv_gate,
        w_query,
        w_key,
        w_value,
        out_conv,
        out_attn,
    )


def plain(tokens, norm_gain, w_conv_value, w_conv_gate, w_query, w_key, w_value, out_conv, out_attn):
    as_float = tokens.astype(jnp.float32)
    normed = (
        as_float
        * lax.rsqrt(jnp.mean(as_float * as_float, axis=-1, keepdims=True) + NORM_EPS)
        * norm_gain.astype(jnp.float32)
    ).astype(jnp.bfloat16)
    pieces = (
        lax.all_gather(w_conv_value, "sp", axis=0, tiled=True),
        lax.all_gather(w_conv_gate, "sp", axis=0, tiled=True),
        lax.all_gather(w_query, "sp", axis=0, tiled=True),
        lax.all_gather(w_key, "sp", axis=0, tiled=True),
        lax.all_gather(w_value, "sp", axis=0, tiled=True),
    )
    projected = tuple(
        (jnp.dot(normed, piece, preferred_element_type=jnp.float32) for piece in pieces)
    )
    conv_value, conv_gate, query_raw, key_raw, value_rows = [
        item.astype(jnp.bfloat16) for item in projected
    ]
    glu = (conv_value.astype(jnp.float32) * jax.nn.sigmoid(conv_gate.astype(jnp.float32))).astype(
        jnp.bfloat16
    )
    cols_conv, cols_attn = (
        lax.all_gather(out_conv, "sp", axis=1, tiled=True),
        lax.all_gather(out_attn, "sp", axis=1, tiled=True),
    )
    return glu, query_raw, key_raw, value_rows, cols_conv, cols_attn


def shards(
    tokens,
    norm_gain,
    w_conv_value,
    w_conv_gate,
    w_query,
    w_key,
    w_value,
    conv_taps,
    ln_gain,
    sinks,
    out_conv,
    out_attn,
):
    row_count = tokens.shape[0]
    whole = fits(lax.axis_size("sp"), w_query.shape, out_conv.shape, row_count)
    glu, query_raw, key_raw, value_rows, cols_conv, cols_attn = (gathered if whole else plain)(
        tokens, norm_gain, w_conv_value, w_conv_gate, w_query, w_key, w_value, out_conv, out_attn
    )
    offset = lax.axis_index("sp") * row_count
    positions = offset + jnp.arange(row_count, dtype=jnp.int32)
    query_heads = query_raw.shape[1] // HEAD_DIM
    key_heads = key_raw.shape[1] // HEAD_DIM
    query = rotate(query_raw.reshape(row_count, query_heads, HEAD_DIM), positions).astype(
        jnp.bfloat16
    )
    key = rotate(key_raw.reshape(row_count, key_heads, HEAD_DIM), positions).astype(jnp.bfloat16)
    reach = conv_taps.shape[0] - 1
    key_tail = key[row_count - WINDOW :]
    value_tail = value_rows.reshape(row_count, key_heads, HEAD_DIM)[row_count - WINDOW :]
    glu_tail = glu[row_count - reach :]
    glu_before = shifted(glu_tail, "sp", 1)
    key_before, value_before = shifted((key_tail, value_tail), "sp", 1)
    extended = jnp.concatenate([glu_before, glu], axis=0).astype(jnp.float32)
    conv_out = jnp.zeros((row_count, glu.shape[1]), jnp.float32)
    for tap in range(reach + 1):
        conv_out = conv_out + conv_taps[tap][None, :] * extended[tap : tap + row_count]
    sum_first = jnp.sum(conv_out, axis=-1)
    sum_second = jnp.sum(conv_out * conv_out, axis=-1)
    total_first, total_second = lax.psum((sum_first, sum_second), "tp")
    mean = (total_first / CONV_CH)[:, None]
    var = (total_second / CONV_CH)[:, None] - mean * mean
    conv_branch = jax.nn.silu(
        (conv_out - mean) * lax.rsqrt(var + CHANNEL_EPS) * ln_gain[None, :]
    ).astype(jnp.bfloat16)
    group = HEADS // KV_HEADS
    blocks = row_count // WINDOW
    q_blocks = query.reshape(blocks, WINDOW, key_heads, group, HEAD_DIM)
    key_blocks = jnp.concatenate([key_before, key], axis=0).reshape(
        blocks + 1, WINDOW, key_heads, HEAD_DIM
    )
    value_all = jnp.concatenate(
        [value_before, value_rows.reshape(row_count, key_heads, HEAD_DIM)], axis=0
    )
    value_blocks = value_all.reshape(blocks + 1, WINDOW, key_heads, HEAD_DIM)
    key_window = jnp.concatenate([key_blocks[:-1], key_blocks[1:]], axis=1)
    value_window = jnp.concatenate([value_blocks[:-1], value_blocks[1:]], axis=1)
    scores = jnp.einsum(
        "nqhgd,nkhd->nhgqk", q_blocks, key_window, preferred_element_type=jnp.float32
    ) * HEAD_DIM ** (-0.5)
    query_index = jnp.arange(WINDOW)[:, None] + WINDOW
    key_index = jnp.arange(2 * WINDOW)[None, :]
    band = (key_index <= query_index) & (query_index - key_index < WINDOW)
    block_index = jnp.arange(blocks)[:, None, None]
    allowed = band[None] & (offset + block_index * WINDOW + key_index[None] - WINDOW >= 0)
    allowed = allowed[:, None, None]
    totals = jnp.sum(jnp.where(allowed, jnp.exp(scores), 0.0), axis=-1)
    totals = totals + jnp.exp(sinks).reshape(1, key_heads, group, 1)
    log_total = jnp.log(totals)
    weights = jnp.where(allowed, jnp.exp(scores - log_total[..., None]), 0.0).astype(jnp.bfloat16)
    attended = jnp.einsum(
        "nhgqk,nkhd->nqhgd", weights, value_window, preferred_element_type=jnp.float32
    )
    attn_branch = attended.astype(jnp.bfloat16).reshape(row_count, query_heads * HEAD_DIM)
    log_sums = log_total.transpose(1, 2, 0, 3).reshape(query_heads, row_count)
    mixed = lax.psum_scatter(
        (
            jnp.dot(conv_branch, cols_conv, preferred_element_type=jnp.float32)
            + jnp.dot(attn_branch, cols_attn, preferred_element_type=jnp.float32)
        ).astype(jnp.bfloat16),
        "tp",
        scatter_dimension=0,
        tiled=True,
    )
    return (mixed, log_sums)


def solution(mesh):
    in_specs = (
        P("sp", None),
        P(),
        P("sp", "tp"),
        P("sp", "tp"),
        P("sp", "tp"),
        P("sp", "tp"),
        P("sp", "tp"),
        P(None, "tp"),
        P("tp"),
        P("tp"),
        P("tp", "sp"),
        P("tp", "sp"),
    )
    out_specs = (P(("sp", "tp"), None), P("tp", "sp"))
    return jax.shard_map(shards, mesh=mesh, in_specs=in_specs, out_specs=out_specs, check_vma=False)
```

```python
import functools

import jax
import jax.numpy as jnp
from jax import lax
from jax.experimental import pallas as pl
from jax.experimental.pallas import tpu as pltpu
from jax.sharding import PartitionSpec as P

CONV_CH = 2048
HEADS = 32
KV_HEADS = 8
HEAD_DIM = 64
WINDOW = 128


NORM_EPS = 1e-06
CHANNEL_EPS = 1e-05
ROPE_BASE = 10000.0


def shifted(value, axis, steps):
    count = lax.axis_size(axis)
    initial, last = (max(0, -steps), min(count, count - steps))
    return lax.ppermute(value, axis, [(source, source + steps) for source in range(initial, last)])


def rotate(heads, positions):
    half_dim = heads.shape[-1] // 2
    inverse = ROPE_BASE ** (-jnp.arange(half_dim, dtype=jnp.float32) / half_dim)
    angles = positions.astype(jnp.float32)[:, None] * inverse[None, :]
    cosine = jnp.cos(angles)[:, None, :]
    sine = jnp.sin(angles)[:, None, :]
    as_float = heads.astype(jnp.float32)
    front_part = as_float[..., :half_dim]
    back_part = as_float[..., half_dim:]
    return jnp.concatenate(
        [front_part * cosine - back_part * sine, back_part * cosine + front_part * sine], axis=-1
    )


def ring_place(index, count):
    half = count // 2
    index = lax.rem(index + 2 * count, count)
    return jnp.where(index < half, 2 * index, 2 * (count - 1 - index) + 1)


class Ring:
    def __init__(self, count, phases, send_sem, recv_sem):
        self.count, self.phases = count, phases
        self.send_sem, self.recv_sem = send_sem, recv_sem
        me = lax.axis_index("sp")
        half = count // 2
        spot = jnp.where(lax.rem(me, 2) == 0, me // 2, count - 1 - me // 2)
        self.spot = spot
        self.peers = (ring_place(spot + 1, count), ring_place(spot - 1, count))

    def owner(self, way, step):
        return ring_place(self.spot - step if way == 0 else self.spot + step, self.count)

    def copy(self, phase, way, piece, step):
        own, place = self.phases[phase][way][piece]
        target = place(self.owner(way, step))
        number = sum(len(p[0]) for p in self.phases[:phase]) + piece
        return pltpu.make_async_remote_copy(
            src_ref=own if step == 0 else target,
            dst_ref=target,
            send_sem=self.send_sem.at[way, number, step],
            recv_sem=self.recv_sem.at[way, number, step],
            device_id={"sp": self.peers[way]},
            device_id_type=pl.DeviceIdType.MESH,
        )

    def arrived(self, phase, way, piece, step):
        own, place = self.phases[phase][way][piece]
        target = place(self.owner(way, step + 1))
        number = sum(len(p[0]) for p in self.phases[:phase]) + piece
        pltpu.make_async_remote_copy(
            src_ref=target,
            dst_ref=target,
            send_sem=self.send_sem.at[way, number, step],
            recv_sem=self.recv_sem.at[way, number, step],
            device_id={"sp": self.peers[way]},
            device_id_type=pl.DeviceIdType.MESH,
        ).wait_recv()

    def begin(self, phase):
        for piece in range(len(self.phases[phase][0])):
            for way in range(2):
                self.copy(phase, way, piece, 0).start()

    def advance(self, phase, step):
        for piece in range(len(self.phases[phase][0])):
            for way in range(2):
                self.arrived(phase, way, piece, step)
                if step + 1 < self.count - 1:
                    self.copy(phase, way, piece, step + 1).start()

    def drain(self):
        for phase in range(len(self.phases)):
            for piece in range(len(self.phases[phase][0])):
                for way in range(2):
                    for step in range(self.count - 1):
                        self.copy(phase, way, piece, step).wait_send()


def layer_kernel(
    count,
    splits,
    tokens,
    norm_gain,
    w_conv_value,
    w_conv_gate,
    w_query,
    w_key,
    w_value,
    taps,
    ln_gain,
    sinks,
    out_conv,
    out_attn,
    cosine,
    sine,
    mixed_out,
    logs_out,
    normed,
    full_cv,
    full_cg,
    full_q,
    full_k,
    full_v,
    full_conv,
    full_attn,
    query,
    key_rows,
    value_rows,
    attn,
    extended,
    glu_tail,
    glu_head,
    conv,
    first,
    second,
    stats,
    stats_in,
    branch,
    share,
    share_in,
    send_sem,
    recv_sem,
    own_sem,
    halo_send,
    halo_recv,
    stat_send,
    stat_recv,
    part_send,
    part_recv,
):
    me, rank = lax.axis_index("sp"), lax.axis_index("tp")
    depth, wide = w_query.shape
    narrow = w_key.shape[1]
    cols = out_conv.shape[1]
    rows = tokens.shape[0]
    lanes = 128
    span = rows // splits
    blocks = rows // WINDOW
    tiles = wide // lanes
    mesh_id = pl.DeviceIdType.MESH

    def by_rows(own, full, low, high):
        return (
            own.at[:, pl.ds(low, high - low)],
            lambda who: full.at[
                pl.ds(pl.multiple_of(who * depth, depth), depth), pl.ds(low, high - low)
            ],
        )

    def by_cols(own, full, way):
        half = cols // 2
        return (
            own.at[:, pl.ds(way * half, half)],
            lambda who: full.at[:, pl.ds(pl.multiple_of(who * cols + way * half, half), half)],
        )

    quarter, middle = wide // 4, wide // 2
    phases = (
        (
            [by_rows(w_query, full_q, i * quarter, (i + 1) * quarter) for i in range(3)],
            [
                by_rows(w_query, full_q, 3 * quarter, wide),
                by_rows(w_key, full_k, 0, narrow),
                by_rows(w_value, full_v, 0, narrow),
            ],
        ),
        (
            [by_rows(w_conv_value, full_cv, i * middle, (i + 1) * middle) for i in range(2)],
            [by_rows(w_conv_gate, full_cg, i * middle, (i + 1) * middle) for i in range(2)],
        ),
        tuple(
            [by_cols(out_conv, full_conv, way), by_cols(out_attn, full_attn, way)]
            for way in range(2)
        ),
    )
    ring = Ring(count, phases, send_sem, recv_sem)
    after, before = lax.rem(me + 1, count), lax.rem(me + count - 1, count)
    barrier = pltpu.get_barrier_semaphore()
    for peer in ring.peers + (after, before):
        pl.semaphore_signal(barrier, inc=1, device_id={"sp": peer}, device_id_type=mesh_id)
    others = [lax.rem(rank + o, splits) for o in range(1, splits)]
    for peer in others:
        pl.semaphore_signal(barrier, inc=1, device_id={"tp": peer}, device_id_type=mesh_id)
    pl.semaphore_wait(barrier, 4 + len(others))
    ring.begin(0)

    mine = pl.ds(pl.multiple_of(me * depth, depth), depth)
    my_cols = pl.ds(pl.multiple_of(me * cols, cols), cols)
    local = [
        pltpu.make_async_copy(own, place, own_sem.at[i])
        for i, (own, place) in enumerate(
            (
                (w_conv_value, full_cv.at[mine]),
                (w_conv_gate, full_cg.at[mine]),
                (w_query, full_q.at[mine]),
                (w_key, full_k.at[mine]),
                (w_value, full_v.at[mine]),
                (out_conv, full_conv.at[:, my_cols]),
                (out_attn, full_attn.at[:, my_cols]),
            )
        )
    ]
    for item in local:
        item.start()

    def forward(source, target, number):
        return pltpu.make_async_remote_copy(
            src_ref=source,
            dst_ref=target,
            send_sem=halo_send.at[number],
            recv_sem=halo_recv.at[number],
            device_id={"sp": after},
            device_id_type=mesh_id,
        )

    tail, head = pl.ds(rows, WINDOW), pl.ds(0, WINDOW)
    halos = (
        forward(key_rows.at[tail], key_rows.at[head], 0),
        forward(value_rows.at[tail], value_rows.at[head], 1),
        forward(glu_tail, glu_head, 2),
    )

    def norm(part):
        take = pl.ds(part * 64, 64)
        x = tokens[take, :].astype(jnp.float32)
        scale = lax.rsqrt(jnp.mean(x * x, axis=-1, keepdims=True) + NORM_EPS)
        normed[take, :] = (x * scale * norm_gain[...].astype(jnp.float32)).astype(jnp.bfloat16)

    def product(take, full):
        return (
            jnp.dot(normed[take, :], full[...], preferred_element_type=jnp.float32)
            .astype(jnp.bfloat16)
            .astype(jnp.float32)
        )

    def turned(x, take):
        lane = lax.broadcasted_iota(jnp.int32, x.shape, 1)
        swapped = jnp.where(
            lane % HEAD_DIM < HEAD_DIM // 2,
            pltpu.roll(x, lanes - HEAD_DIM // 2, 1),
            pltpu.roll(x, HEAD_DIM // 2, 1),
        )
        return (x * cosine[take, :] + swapped * sine[take, :]).astype(jnp.bfloat16)

    def attention_side(part):
        take = pl.ds(part * WINDOW, WINDOW)
        put = pl.ds((part + 1) * WINDOW, WINDOW)
        q = product(take, full_q)
        for tile in range(tiles):
            query[take, pl.ds(tile * lanes, lanes)] = turned(
                q[:, tile * lanes : (tile + 1) * lanes], take
            )
        key_rows[put, :] = turned(product(take, full_k), take)
        value_rows[put, :] = product(take, full_v).astype(jnp.bfloat16)

    def attend(part):
        take = pl.ds(part * WINDOW, WINDOW)
        window = pl.ds(part * WINDOW, 2 * WINDOW)
        low = lax.broadcasted_iota(jnp.int32, (2 * WINDOW, lanes), 1) < HEAD_DIM
        low_q = lax.broadcasted_iota(jnp.int32, (WINDOW, lanes), 1) < HEAD_DIM
        keys = key_rows[window, :].astype(jnp.float32)
        values = value_rows[window, :].astype(jnp.float32)
        keys_turned, values_turned = pltpu.roll(keys, HEAD_DIM, 1), pltpu.roll(values, HEAD_DIM, 1)
        group = wide // narrow
        shape = (group * WINDOW, 2 * WINDOW)
        row = lax.broadcasted_iota(jnp.int32, shape, 0) % WINDOW
        col = lax.broadcasted_iota(jnp.int32, shape, 1)
        start = me * rows + (part - 1) * WINDOW
        allowed = (col > row) & (col <= row + WINDOW) & (start + col >= 0)
        lane = lax.broadcasted_iota(jnp.int32, (WINDOW, lanes), 1)
        totals = jnp.exp(sinks[...]) + jnp.zeros((WINDOW, lanes), jnp.float32)
        all_scores = []
        for head in range(2):
            two = jnp.where(low if head == 0 else ~low, keys, keys_turned).astype(jnp.bfloat16)
            stacked = []
            for pair in range(group // 2):
                tile = head * (group // 2) + pair
                q = query[take, pl.ds(tile * lanes, lanes)].astype(jnp.float32)
                stacked += [jnp.where(low_q, q, 0.0), jnp.where(low_q, 0.0, q)]
            q_all = jnp.concatenate(stacked, axis=0).astype(jnp.bfloat16)
            scores = lax.dot_general(
                q_all, two, (((1,), (1,)), ((), ())), preferred_element_type=jnp.float32
            ) * HEAD_DIM ** (-0.5)
            all_scores.append(scores)
            sums = jnp.sum(jnp.where(allowed, jnp.exp(scores), 0.0), axis=-1, keepdims=True)
            for i in range(group):
                totals = totals + jnp.where(
                    lane == head * group + i, sums[i * WINDOW : (i + 1) * WINDOW], 0.0
                )
        logs = jnp.log(totals)
        logs_out[:, pl.ds(part * WINDOW, WINDOW)] = logs.T[: logs_out.shape[0]]
        for head in range(2):
            two = jnp.where(low if head == 0 else ~low, values, values_turned).astype(jnp.bfloat16)
            level = jnp.concatenate(
                [logs[:, head * group + i : head * group + i + 1] for i in range(group)], axis=0
            )
            weights = jnp.where(allowed, jnp.exp(all_scores[head] - level), 0.0)
            got = jnp.dot(weights.astype(jnp.bfloat16), two, preferred_element_type=jnp.float32)
            for pair in range(group // 2):
                tile = head * (group // 2) + pair
                one = got[2 * pair * WINDOW : (2 * pair + 1) * WINDOW]
                other = got[(2 * pair + 1) * WINDOW : (2 * pair + 2) * WINDOW]
                attn[take, pl.ds(tile * lanes, lanes)] = jnp.where(low_q, one, other).astype(
                    jnp.bfloat16
                )

    edge = glu_tail.shape[0]

    def conv_side(part):
        take = pl.ds(part * WINDOW, WINDOW)
        glu = (product(take, full_cv) * jax.nn.sigmoid(product(take, full_cg))).astype(jnp.bfloat16)
        if part == blocks - 1:
            glu_tail[...] = glu[WINDOW - edge :]
        glu = glu.astype(jnp.float32)
        for tile in range(tiles):
            extended[tile, pl.ds(edge + part * WINDOW, WINDOW), :] = glu[
                :, tile * lanes : (tile + 1) * lanes
            ]

    def take_halo():
        halos[2].wait_recv()
        for tile in range(tiles):
            got = glu_head[:, pl.ds(tile * lanes, lanes)].astype(jnp.float32)
            extended[tile, pl.ds(0, edge), :] = jnp.where(me > 0, got, 0.0)

    def convolve(tile):
        reach = taps.shape[0]
        block = 64

        @pl.loop(0, rows // block)
        def _(part):
            base = pl.multiple_of(part * block, block)
            total = jnp.zeros((block, lanes), jnp.float32)
            for j in range(reach):
                total = total + taps[pl.ds(j, 1), pl.ds(tile * lanes, lanes)] * extended[
                    tile, pl.ds(base + (edge - reach + 1 + j), block), :
                ]
            take = pl.ds(base, block)
            conv[tile, take, :] = total
            if tile == 0:
                first[take, :] = total
                second[take, :] = total * total
            else:
                first[take, :] = first[take, :] + total
                second[take, :] = second[take, :] + total * total

    def stat_copy(o):
        return pltpu.make_async_remote_copy(
            src_ref=stats,
            dst_ref=stats_in.at[o],
            send_sem=stat_send.at[o],
            recv_sem=stat_recv.at[o],
            device_id={"tp": others[o]},
            device_id_type=mesh_id,
        )

    def send_stats():
        lane = lax.broadcasted_iota(jnp.int32, (WINDOW, lanes), 1)
        mat = jnp.zeros((WINDOW, lanes), jnp.float32)
        for part in range(blocks):
            take = pl.ds(part * WINDOW, WINDOW)
            mat = jnp.where(lane == 2 * part, jnp.sum(first[take, :], -1, keepdims=True), mat)
            mat = jnp.where(lane == 2 * part + 1, jnp.sum(second[take, :], -1, keepdims=True), mat)
        stats[...] = mat
        for o in range(splits - 1):
            stat_copy(o).start()

    def finish_conv():
        total = stats[...]
        for o in range(splits - 1):
            stat_copy(o).wait_recv()
            total = total + stats_in[o]
        total = total / CONV_CH
        for part in range(blocks):
            take = pl.ds(part * WINDOW, WINDOW)
            mean = total[:, 2 * part : 2 * part + 1]
            scale = lax.rsqrt(total[:, 2 * part + 1 : 2 * part + 2] - mean * mean + CHANNEL_EPS)
            for tile in range(tiles):
                at = pl.ds(tile * lanes, lanes)
                value = (conv[tile, take, :] - mean) * scale * ln_gain[:, at]
                branch[take, at] = (value * jax.nn.sigmoid(value)).astype(jnp.bfloat16)

    def part_copy(way, step, o):
        half = cols // 2
        at = pl.ds(pl.multiple_of(ring.owner(way, step) * cols + way * half, half), half)
        return pltpu.make_async_remote_copy(
            src_ref=share.at[pl.ds(pl.multiple_of(others[o] * span, span), span), at],
            dst_ref=share_in.at[o, :, at],
            send_sem=part_send.at[way, step, o],
            recv_sem=part_recv.at[way, step, o],
            device_id={"tp": others[o]},
            device_id_type=mesh_id,
        )

    def project_out(step):
        half = cols // 2
        for way in range(2):
            at = pl.ds(pl.multiple_of(ring.owner(way, step) * cols + way * half, half), half)
            share[:, at] = (
                jnp.dot(branch[...], full_conv[:, at], preferred_element_type=jnp.float32)
                + jnp.dot(attn[...], full_attn[:, at], preferred_element_type=jnp.float32)
            ).astype(jnp.bfloat16)
        for way in range(2):
            for o in range(splits - 1):
                part_copy(way, step, o).start()

    def run(phase, plan):
        for step in range(count - 1):
            for item in plan[step] if step < len(plan) else ():
                item()
            ring.advance(phase, step)
            if step == count - 3 and phase + 1 < len(phases):
                ring.begin(phase + 1)

    each = functools.partial

    def spread(items, steps):
        return [
            items[i * len(items) // steps : (i + 1) * len(items) // steps] for i in range(steps)
        ]

    run(0, spread([each(norm, i) for i in range(rows // 64)], count - 1))
    for item in local:
        item.wait()

    def send_rows():
        halos[0].start()
        halos[1].start()

    def take_rows():
        halos[0].wait_recv()
        halos[1].wait_recv()

    sides = [each(attention_side, i) for i in range(blocks)]
    sides.append(send_rows)
    sides += [each(attend, i) for i in range(1, blocks)]
    sides += [take_rows, each(attend, 0)]
    run(1, spread(sides, count - 1))
    opening = [each(conv_side, i) for i in range(blocks)] + [halos[2].start]
    middle_work = [take_halo] + [each(convolve, i) for i in range(tiles)] + [send_stats]
    plan = [opening, middle_work, [finish_conv]]
    plan.append([each(project_out, i) for i in range(4)])
    plan += [[each(project_out, i)] for i in range(4, count - 1)]
    plan = plan if count > 4 else [opening + middle_work + [finish_conv]]
    run(2, plan)
    for step in range(count - 1 if count > 4 else 0, count):
        project_out(step)
    ring.drain()
    for halo in halos:
        halo.wait_send()
    for o in range(splits - 1):
        stat_copy(o).wait_send()
    for step in range(count):
        for way in range(2):
            for o in range(splits - 1):
                part_copy(way, step, o).wait()
    total = share[pl.ds(pl.multiple_of(rank * span, span), span), :].astype(jnp.float32)
    for o in range(splits - 1):
        total = total + share_in[o].astype(jnp.float32)
    mixed_out[...] = total.astype(jnp.bfloat16)


def fits(count, splits, tokens, w_query, w_key, out_conv):
    rows, width = tokens.shape
    depth, wide = w_query.shape
    if depth % 128 or wide % 512 or out_conv.shape[1] % 256 or rows % (128 * splits):
        return False
    if w_key.shape[1] != 2 * HEAD_DIM or wide != 4 * w_key.shape[1] or rows > 64 * 128:
        return False
    return count % 2 == 0 and 3 < count <= 16 and splits > 1


def one_kernel(
    tokens,
    norm_gain,
    w_conv_value,
    w_conv_gate,
    w_query,
    w_key,
    w_value,
    conv_taps,
    ln_gain,
    sinks,
    out_conv,
    out_attn,
):
    count, splits = lax.axis_size("sp"), lax.axis_size("tp")
    rows, width = tokens.shape
    wide, narrow = w_query.shape[1], w_key.shape[1]
    long = out_conv.shape[0]
    full_cols = count * out_conv.shape[1]
    tiles = wide // 128
    edge = 32
    span = rows // splits
    half_dim = HEAD_DIM // 2
    inverse = ROPE_BASE ** (-jnp.arange(half_dim, dtype=jnp.float32) / half_dim)
    positions = lax.axis_index("sp") * rows + jnp.arange(rows, dtype=jnp.int32)
    angles = positions.astype(jnp.float32)[:, None] * jnp.tile(inverse, 4)[None, :]
    sign = jnp.tile(jnp.repeat(jnp.array([-1.0, 1.0], jnp.float32), half_dim), 2)
    cosine, sine = jnp.cos(angles), jnp.sin(angles) * sign[None, :]
    vmem = pl.BlockSpec(memory_space=pltpu.VMEM)
    low = lambda *dims: pltpu.VMEM(dims, jnp.bfloat16)
    high = lambda *dims: pltpu.VMEM(dims, jnp.float32)
    dma = lambda *dims: pltpu.SemaphoreType.DMA(dims)
    return pl.pallas_call(
        functools.partial(layer_kernel, count, splits),
        out_shape=(
            jax.ShapeDtypeStruct((span, full_cols), jnp.bfloat16),
            jax.ShapeDtypeStruct((wide // HEAD_DIM, rows), jnp.float32),
        ),
        in_specs=[vmem] * 14,
        out_specs=(vmem,) * 2,
        scratch_shapes=[
            low(rows, width),
            low(width, wide),
            low(width, wide),
            low(width, wide),
            low(width, narrow),
            low(width, narrow),
            low(long, full_cols),
            low(long, full_cols),
            low(rows, wide),
            low(rows + WINDOW, narrow),
            low(rows + WINDOW, narrow),
            low(rows, wide),
            high(tiles, rows + edge, 128),
            low(edge, wide),
            low(edge, wide),
            high(tiles, rows, 128),
            high(rows, 128),
            high(rows, 128),
            high(128, 128),
            high(splits - 1, 128, 128),
            low(rows, wide),
            low(rows, full_cols),
            low(splits - 1, span, full_cols),
            dma(2, 7, count - 1),
            dma(2, 7, count - 1),
            dma(7),
            dma(3),
            dma(3),
            dma(splits - 1),
            dma(splits - 1),
            dma(2, count, splits - 1),
            dma(2, count, splits - 1),
        ],
        compiler_params=pltpu.CompilerParams(collective_id=0, has_side_effects=True),
        name="layer",
    )(
        tokens,
        norm_gain.reshape(1, width),
        w_conv_value,
        w_conv_gate,
        w_query,
        w_key,
        w_value,
        conv_taps,
        ln_gain.reshape(1, -1),
        jnp.pad(sinks, (0, 128 - sinks.shape[0])).reshape(1, 128),
        out_conv,
        out_attn,
        cosine,
        sine,
    )


def plain(tokens, norm_gain, w_conv_value, w_conv_gate, w_query, w_key, w_value, out_conv, out_attn):
    as_float = tokens.astype(jnp.float32)
    normed = (
        as_float
        * lax.rsqrt(jnp.mean(as_float * as_float, axis=-1, keepdims=True) + NORM_EPS)
        * norm_gain.astype(jnp.float32)
    ).astype(jnp.bfloat16)
    pieces = (
        lax.all_gather(w_conv_value, "sp", axis=0, tiled=True),
        lax.all_gather(w_conv_gate, "sp", axis=0, tiled=True),
        lax.all_gather(w_query, "sp", axis=0, tiled=True),
        lax.all_gather(w_key, "sp", axis=0, tiled=True),
        lax.all_gather(w_value, "sp", axis=0, tiled=True),
    )
    projected = tuple(
        (jnp.dot(normed, piece, preferred_element_type=jnp.float32) for piece in pieces)
    )
    conv_value, conv_gate, query_raw, key_raw, value_rows = [
        item.astype(jnp.bfloat16) for item in projected
    ]
    glu = (conv_value.astype(jnp.float32) * jax.nn.sigmoid(conv_gate.astype(jnp.float32))).astype(
        jnp.bfloat16
    )
    cols_conv, cols_attn = (
        lax.all_gather(out_conv, "sp", axis=1, tiled=True),
        lax.all_gather(out_attn, "sp", axis=1, tiled=True),
    )
    return glu, query_raw, key_raw, value_rows, cols_conv, cols_attn


def shards(
    tokens,
    norm_gain,
    w_conv_value,
    w_conv_gate,
    w_query,
    w_key,
    w_value,
    conv_taps,
    ln_gain,
    sinks,
    out_conv,
    out_attn,
):
    row_count = tokens.shape[0]
    if fits(lax.axis_size("sp"), lax.axis_size("tp"), tokens, w_query, w_key, out_conv):
        return one_kernel(
            tokens,
            norm_gain,
            w_conv_value,
            w_conv_gate,
            w_query,
            w_key,
            w_value,
            conv_taps,
            ln_gain,
            sinks,
            out_conv,
            out_attn,
        )
    glu, query_raw, key_raw, value_rows, cols_conv, cols_attn = plain(
        tokens, norm_gain, w_conv_value, w_conv_gate, w_query, w_key, w_value, out_conv, out_attn
    )
    offset = lax.axis_index("sp") * row_count
    positions = offset + jnp.arange(row_count, dtype=jnp.int32)
    query_heads = query_raw.shape[1] // HEAD_DIM
    key_heads = key_raw.shape[1] // HEAD_DIM
    query = rotate(query_raw.reshape(row_count, query_heads, HEAD_DIM), positions).astype(
        jnp.bfloat16
    )
    key = rotate(key_raw.reshape(row_count, key_heads, HEAD_DIM), positions).astype(jnp.bfloat16)
    reach = conv_taps.shape[0] - 1
    key_tail = key[row_count - WINDOW :]
    value_tail = value_rows.reshape(row_count, key_heads, HEAD_DIM)[row_count - WINDOW :]
    glu_tail = glu[row_count - reach :]
    glu_before = shifted(glu_tail, "sp", 1)
    key_before, value_before = shifted((key_tail, value_tail), "sp", 1)
    extended = jnp.concatenate([glu_before, glu], axis=0).astype(jnp.float32)
    conv_out = jnp.zeros((row_count, glu.shape[1]), jnp.float32)
    for tap in range(reach + 1):
        conv_out = conv_out + conv_taps[tap][None, :] * extended[tap : tap + row_count]
    sum_first = jnp.sum(conv_out, axis=-1)
    sum_second = jnp.sum(conv_out * conv_out, axis=-1)
    total_first, total_second = lax.psum((sum_first, sum_second), "tp")
    mean = (total_first / CONV_CH)[:, None]
    var = (total_second / CONV_CH)[:, None] - mean * mean
    conv_branch = jax.nn.silu(
        (conv_out - mean) * lax.rsqrt(var + CHANNEL_EPS) * ln_gain[None, :]
    ).astype(jnp.bfloat16)
    group = HEADS // KV_HEADS
    blocks = row_count // WINDOW
    q_blocks = query.reshape(blocks, WINDOW, key_heads, group, HEAD_DIM)
    key_blocks = jnp.concatenate([key_before, key], axis=0).reshape(
        blocks + 1, WINDOW, key_heads, HEAD_DIM
    )
    value_all = jnp.concatenate(
        [value_before, value_rows.reshape(row_count, key_heads, HEAD_DIM)], axis=0
    )
    value_blocks = value_all.reshape(blocks + 1, WINDOW, key_heads, HEAD_DIM)
    key_window = jnp.concatenate([key_blocks[:-1], key_blocks[1:]], axis=1)
    value_window = jnp.concatenate([value_blocks[:-1], value_blocks[1:]], axis=1)
    scores = jnp.einsum(
        "nqhgd,nkhd->nhgqk", q_blocks, key_window, preferred_element_type=jnp.float32
    ) * HEAD_DIM ** (-0.5)
    query_index = jnp.arange(WINDOW)[:, None] + WINDOW
    key_index = jnp.arange(2 * WINDOW)[None, :]
    band = (key_index <= query_index) & (query_index - key_index < WINDOW)
    block_index = jnp.arange(blocks)[:, None, None]
    allowed = band[None] & (offset + block_index * WINDOW + key_index[None] - WINDOW >= 0)
    allowed = allowed[:, None, None]
    totals = jnp.sum(jnp.where(allowed, jnp.exp(scores), 0.0), axis=-1)
    totals = totals + jnp.exp(sinks).reshape(1, key_heads, group, 1)
    log_total = jnp.log(totals)
    weights = jnp.where(allowed, jnp.exp(scores - log_total[..., None]), 0.0).astype(jnp.bfloat16)
    attended = jnp.einsum(
        "nhgqk,nkhd->nqhgd", weights, value_window, preferred_element_type=jnp.float32
    )
    attn_branch = attended.astype(jnp.bfloat16).reshape(row_count, query_heads * HEAD_DIM)
    log_sums = log_total.transpose(1, 2, 0, 3).reshape(query_heads, row_count)
    mixed = lax.psum_scatter(
        (
            jnp.dot(conv_branch, cols_conv, preferred_element_type=jnp.float32)
            + jnp.dot(attn_branch, cols_attn, preferred_element_type=jnp.float32)
        ).astype(jnp.bfloat16),
        "tp",
        scatter_dimension=0,
        tiled=True,
    )
    return (mixed, log_sums)


def solution(mesh):
    in_specs = (
        P("sp", None),
        P(),
        P("sp", "tp"),
        P("sp", "tp"),
        P("sp", "tp"),
        P("sp", "tp"),
        P("sp", "tp"),
        P(None, "tp"),
        P("tp"),
        P("tp"),
        P("tp", "sp"),
        P("tp", "sp"),
    )
    out_specs = (P(("sp", "tp"), None), P("tp", "sp"))
    return jax.shard_map(shards, mesh=mesh, in_specs=in_specs, out_specs=out_specs, check_vma=False)
```

```python
import functools

import jax
import jax.numpy as jnp
import numpy as np
from jax import lax
from jax.experimental import pallas as pl
from jax.experimental.pallas import tpu as pltpu
from jax.sharding import PartitionSpec as P

CONV_CH = 2048
HEADS = 32
KV_HEADS = 8
HEAD_DIM = 64
WINDOW = 128


NORM_EPS = 1e-06
CHANNEL_EPS = 1e-05
ROPE_BASE = 10000.0


def shifted(value, axis, steps):
    count = lax.axis_size(axis)
    initial, last = (max(0, -steps), min(count, count - steps))
    return lax.ppermute(value, axis, [(source, source + steps) for source in range(initial, last)])


def rotate(heads, positions):
    half_dim = heads.shape[-1] // 2
    inverse = ROPE_BASE ** (-jnp.arange(half_dim, dtype=jnp.float32) / half_dim)
    angles = positions.astype(jnp.float32)[:, None] * inverse[None, :]
    cosine = jnp.cos(angles)[:, None, :]
    sine = jnp.sin(angles)[:, None, :]
    as_float = heads.astype(jnp.float32)
    front_part = as_float[..., :half_dim]
    back_part = as_float[..., half_dim:]
    return jnp.concatenate(
        [front_part * cosine - back_part * sine, back_part * cosine + front_part * sine], axis=-1
    )


def ring_place(index, count):
    half = count // 2
    index = lax.rem(index + 2 * count, count)
    return jnp.where(index < half, 2 * index, 2 * (count - 1 - index) + 1)


class Ring:
    def __init__(self, count, phases, send_sem, recv_sem):
        self.count, self.phases = count, phases
        self.send_sem, self.recv_sem = send_sem, recv_sem
        me = lax.axis_index("sp")
        half = count // 2
        spot = jnp.where(lax.rem(me, 2) == 0, me // 2, count - 1 - me // 2)
        self.spot = spot
        self.peers = (ring_place(spot + 1, count), ring_place(spot - 1, count))

    def owner(self, way, step):
        return ring_place(self.spot - step if way == 0 else self.spot + step, self.count)

    def copy(self, phase, way, piece, step):
        own, place = self.phases[phase][way][piece]
        target = place(self.owner(way, step))
        number = sum(len(p[0]) for p in self.phases[:phase]) + piece
        return pltpu.make_async_remote_copy(
            src_ref=own if step == 0 else target,
            dst_ref=target,
            send_sem=self.send_sem.at[way, number, step],
            recv_sem=self.recv_sem.at[way, number, step],
            device_id={"sp": self.peers[way]},
            device_id_type=pl.DeviceIdType.MESH,
        )

    def arrived(self, phase, way, piece, step):
        own, place = self.phases[phase][way][piece]
        target = place(self.owner(way, step + 1))
        number = sum(len(p[0]) for p in self.phases[:phase]) + piece
        pltpu.make_async_remote_copy(
            src_ref=target,
            dst_ref=target,
            send_sem=self.send_sem.at[way, number, step],
            recv_sem=self.recv_sem.at[way, number, step],
            device_id={"sp": self.peers[way]},
            device_id_type=pl.DeviceIdType.MESH,
        ).wait_recv()

    def begin(self, phase):
        for piece in range(len(self.phases[phase][0])):
            for way in range(2):
                self.copy(phase, way, piece, 0).start()

    def advance(self, phase, step, piece):
        for way in range(2):
            self.arrived(phase, way, piece, step)
            if step + 1 < self.count - 1:
                self.copy(phase, way, piece, step + 1).start()

    def drain(self):
        for phase in range(len(self.phases)):
            for piece in range(len(self.phases[phase][0])):
                for way in range(2):
                    for step in range(self.count - 1):
                        self.copy(phase, way, piece, step).wait_send()


def layer_kernel(
    count,
    splits,
    tokens,
    norm_gain,
    w_conv_value,
    w_conv_gate,
    w_query,
    w_key,
    w_value,
    taps,
    ln_gain,
    sinks,
    out_conv,
    out_attn,
    mixed_out,
    logs_out,
    normed,
    full_cv,
    full_cg,
    full_q,
    full_k,
    full_v,
    full_conv,
    full_attn,
    query,
    key_rows,
    value_rows,
    attn,
    extended,
    glu_tail,
    glu_head,
    conv,
    first,
    second,
    stats,
    stats_in,
    branch,
    share,
    share_in,
    send_sem,
    recv_sem,
    own_sem,
    halo_send,
    halo_recv,
    stat_send,
    stat_recv,
    part_send,
    part_recv,
    cosine,
    sine,
):
    me, rank = lax.axis_index("sp"), lax.axis_index("tp")
    depth, wide = w_query.shape
    narrow = w_key.shape[1]
    cols = out_conv.shape[1]
    rows = tokens.shape[0]
    lanes = 128
    span = rows // splits
    blocks = rows // WINDOW
    tiles = wide // lanes
    mesh_id = pl.DeviceIdType.MESH

    def by_rows(own, full, low, high):
        return (
            own.at[:, pl.ds(low, high - low)],
            lambda who: full.at[
                pl.ds(pl.multiple_of(who * depth, depth), depth), pl.ds(low, high - low)
            ],
        )

    def by_cols(own, full, way):
        half = cols // 2
        return (
            own.at[:, pl.ds(way * half, half)],
            lambda who: full.at[:, pl.ds(pl.multiple_of(who * cols + way * half, half), half)],
        )

    quarter, middle = wide // 4, wide // 2
    phases = (
        (
            [by_rows(w_query, full_q, i * quarter, (i + 1) * quarter) for i in range(3)],
            [
                by_rows(w_query, full_q, 3 * quarter, wide),
                by_rows(w_key, full_k, 0, narrow),
                by_rows(w_value, full_v, 0, narrow),
            ],
        ),
        (
            [by_rows(w_conv_value, full_cv, i * middle, (i + 1) * middle) for i in range(2)],
            [by_rows(w_conv_gate, full_cg, i * middle, (i + 1) * middle) for i in range(2)],
        ),
        tuple(
            [by_cols(out_conv, full_conv, way), by_cols(out_attn, full_attn, way)]
            for way in range(2)
        ),
    )
    ring = Ring(count, phases, send_sem, recv_sem)
    after, before = lax.rem(me + 1, count), lax.rem(me + count - 1, count)
    barrier = pltpu.get_barrier_semaphore()
    for peer in ring.peers + (after, before):
        pl.semaphore_signal(barrier, inc=1, device_id={"sp": peer}, device_id_type=mesh_id)
    others = [lax.rem(rank + o, splits) for o in range(1, splits)]
    for peer in others:
        pl.semaphore_signal(barrier, inc=1, device_id={"tp": peer}, device_id_type=mesh_id)
    pl.semaphore_wait(barrier, 4 + len(others))
    ring.begin(0)

    mine = pl.ds(pl.multiple_of(me * depth, depth), depth)
    my_cols = pl.ds(pl.multiple_of(me * cols, cols), cols)
    local = [
        pltpu.make_async_copy(own, place, own_sem.at[i])
        for i, (own, place) in enumerate(
            (
                (w_conv_value, full_cv.at[mine]),
                (w_conv_gate, full_cg.at[mine]),
                (w_query, full_q.at[mine]),
                (w_key, full_k.at[mine]),
                (w_value, full_v.at[mine]),
                (out_conv, full_conv.at[:, my_cols]),
                (out_attn, full_attn.at[:, my_cols]),
            )
        )
    ]
    for item in local:
        item.start()

    def forward(source, target, number):
        return pltpu.make_async_remote_copy(
            src_ref=source,
            dst_ref=target,
            send_sem=halo_send.at[number],
            recv_sem=halo_recv.at[number],
            device_id={"sp": after},
            device_id_type=mesh_id,
        )

    tail, head = pl.ds(rows, WINDOW), pl.ds(0, WINDOW)
    halos = (
        forward(key_rows.at[tail], key_rows.at[head], 0),
        forward(value_rows.at[tail], value_rows.at[head], 1),
        forward(glu_tail, glu_head, 2),
    )

    def norm(part):
        take = pl.ds(part * 64, 64)
        x = tokens[take, :].astype(jnp.float32)
        scale = lax.rsqrt(jnp.mean(x * x, axis=-1, keepdims=True) + NORM_EPS)
        normed[take, :] = (x * scale * norm_gain[...].astype(jnp.float32)[None, :]).astype(jnp.bfloat16)

    def table(part):
        take = pl.ds(part * WINDOW, WINDOW)
        shape = (WINDOW, lanes)
        half_dim = HEAD_DIM // 2
        lane = lax.broadcasted_iota(jnp.int32, shape, 1)
        place = me * rows + part * WINDOW + lax.broadcasted_iota(jnp.int32, shape, 0)
        inverse = jnp.zeros(shape, jnp.float32)
        for i in range(half_dim):
            exact = float(np.float32(ROPE_BASE ** (-i / half_dim)))
            inverse = jnp.where(lane % half_dim == i, exact, inverse)
        angles = place.astype(jnp.float32) * inverse
        cosine[take, :] = jnp.cos(angles)
        sine[take, :] = jnp.where(lane % HEAD_DIM < half_dim, -jnp.sin(angles), jnp.sin(angles))

    def product(take, full):
        return (
            jnp.dot(normed[take, :], full[...], preferred_element_type=jnp.float32)
            .astype(jnp.bfloat16)
            .astype(jnp.float32)
        )

    def turned(x, take):
        lane = lax.broadcasted_iota(jnp.int32, x.shape, 1)
        swapped = jnp.where(
            lane % HEAD_DIM < HEAD_DIM // 2,
            pltpu.roll(x, lanes - HEAD_DIM // 2, 1),
            pltpu.roll(x, HEAD_DIM // 2, 1),
        )
        return (x * cosine[take, :] + swapped * sine[take, :]).astype(jnp.bfloat16)

    def attention_side(part):
        take = pl.ds(part * WINDOW, WINDOW)
        put = pl.ds((part + 1) * WINDOW, WINDOW)
        q = product(take, full_q)
        for tile in range(tiles):
            query[take, pl.ds(tile * lanes, lanes)] = turned(
                q[:, tile * lanes : (tile + 1) * lanes], take
            )
        key_rows[put, :] = turned(product(take, full_k), take)
        value_rows[put, :] = product(take, full_v).astype(jnp.bfloat16)

    def attend(part):
        take = pl.ds(part * WINDOW, WINDOW)
        window = pl.ds(part * WINDOW, 2 * WINDOW)
        low = lax.broadcasted_iota(jnp.int32, (2 * WINDOW, lanes), 1) < HEAD_DIM
        low_q = lax.broadcasted_iota(jnp.int32, (WINDOW, lanes), 1) < HEAD_DIM
        keys = key_rows[window, :].astype(jnp.float32)
        values = value_rows[window, :].astype(jnp.float32)
        keys_turned, values_turned = pltpu.roll(keys, HEAD_DIM, 1), pltpu.roll(values, HEAD_DIM, 1)
        group = wide // narrow
        shape = (group * WINDOW, 2 * WINDOW)
        row = lax.broadcasted_iota(jnp.int32, shape, 0) % WINDOW
        col = lax.broadcasted_iota(jnp.int32, shape, 1)
        start = me * rows + (part - 1) * WINDOW
        allowed = (col > row) & (col <= row + WINDOW) & (start + col >= 0)
        lane = lax.broadcasted_iota(jnp.int32, (WINDOW, lanes), 1)
        totals = jnp.zeros((WINDOW, lanes), jnp.float32)
        for i in range(2 * group):
            totals = jnp.where(lane == i, sinks[i], totals)
        totals = jnp.exp(totals)
        all_scores = []
        for head in range(2):
            two = jnp.where(low if head == 0 else ~low, keys, keys_turned).astype(jnp.bfloat16)
            stacked = []
            for pair in range(group // 2):
                tile = head * (group // 2) + pair
                q = query[take, pl.ds(tile * lanes, lanes)].astype(jnp.float32)
                stacked += [jnp.where(low_q, q, 0.0), jnp.where(low_q, 0.0, q)]
            q_all = jnp.concatenate(stacked, axis=0).astype(jnp.bfloat16)
            scores = lax.dot_general(
                q_all, two, (((1,), (1,)), ((), ())), preferred_element_type=jnp.float32
            ) * HEAD_DIM ** (-0.5)
            all_scores.append(scores)
            sums = jnp.sum(jnp.where(allowed, jnp.exp(scores), 0.0), axis=-1, keepdims=True)
            for i in range(group):
                totals = totals + jnp.where(
                    lane == head * group + i, sums[i * WINDOW : (i + 1) * WINDOW], 0.0
                )
        logs = jnp.log(totals)
        logs_out[:, pl.ds(part * WINDOW, WINDOW)] = logs.T[: logs_out.shape[0]]
        for head in range(2):
            two = jnp.where(low if head == 0 else ~low, values, values_turned).astype(jnp.bfloat16)
            level = jnp.concatenate(
                [logs[:, head * group + i : head * group + i + 1] for i in range(group)], axis=0
            )
            weights = jnp.where(allowed, jnp.exp(all_scores[head] - level), 0.0)
            got = jnp.dot(weights.astype(jnp.bfloat16), two, preferred_element_type=jnp.float32)
            for pair in range(group // 2):
                tile = head * (group // 2) + pair
                one = got[2 * pair * WINDOW : (2 * pair + 1) * WINDOW]
                other = got[(2 * pair + 1) * WINDOW : (2 * pair + 2) * WINDOW]
                attn[take, pl.ds(tile * lanes, lanes)] = jnp.where(low_q, one, other).astype(
                    jnp.bfloat16
                )

    edge = glu_tail.shape[0]

    def conv_side(part):
        take = pl.ds(part * WINDOW, WINDOW)
        glu = (product(take, full_cv) * jax.nn.sigmoid(product(take, full_cg))).astype(jnp.bfloat16)
        if part == blocks - 1:
            glu_tail[...] = glu[WINDOW - edge :]
        glu = glu.astype(jnp.float32)
        for tile in range(tiles):
            extended[tile, pl.ds(edge + part * WINDOW, WINDOW), :] = glu[
                :, tile * lanes : (tile + 1) * lanes
            ]

    def take_halo():
        halos[2].wait_recv()
        for tile in range(tiles):
            got = glu_head[:, pl.ds(tile * lanes, lanes)].astype(jnp.float32)
            extended[tile, pl.ds(0, edge), :] = jnp.where(me > 0, got, 0.0)

    def convolve(tile):
        reach = taps.shape[0]
        block = 64

        @pl.loop(0, rows // block)
        def _(part):
            base = pl.multiple_of(part * block, block)
            total = jnp.zeros((block, lanes), jnp.float32)
            for j in range(reach):
                total = total + taps[pl.ds(j, 1), pl.ds(tile * lanes, lanes)] * extended[
                    tile, pl.ds(base + (edge - reach + 1 + j), block), :
                ]
            take = pl.ds(base, block)
            conv[tile, take, :] = total
            if tile == 0:
                first[take, :] = total
                second[take, :] = total * total
            else:
                first[take, :] = first[take, :] + total
                second[take, :] = second[take, :] + total * total

    def stat_copy(o):
        return pltpu.make_async_remote_copy(
            src_ref=stats,
            dst_ref=stats_in.at[o],
            send_sem=stat_send.at[o],
            recv_sem=stat_recv.at[o],
            device_id={"tp": others[o]},
            device_id_type=mesh_id,
        )

    def send_stats():
        lane = lax.broadcasted_iota(jnp.int32, (WINDOW, lanes), 1)
        mat = jnp.zeros((WINDOW, lanes), jnp.float32)
        for part in range(blocks):
            take = pl.ds(part * WINDOW, WINDOW)
            mat = jnp.where(lane == 2 * part, jnp.sum(first[take, :], -1, keepdims=True), mat)
            mat = jnp.where(lane == 2 * part + 1, jnp.sum(second[take, :], -1, keepdims=True), mat)
        stats[...] = mat
        for o in range(splits - 1):
            stat_copy(o).start()

    def finish_conv():
        total = stats[...]
        for o in range(splits - 1):
            stat_copy(o).wait_recv()
            total = total + stats_in[o]
        total = total / CONV_CH
        for part in range(blocks):
            take = pl.ds(part * WINDOW, WINDOW)
            mean = total[:, 2 * part : 2 * part + 1]
            scale = lax.rsqrt(total[:, 2 * part + 1 : 2 * part + 2] - mean * mean + CHANNEL_EPS)
            for tile in range(tiles):
                at = pl.ds(tile * lanes, lanes)
                value = (conv[tile, take, :] - mean) * scale * ln_gain[:, at]
                branch[take, at] = (value * jax.nn.sigmoid(value)).astype(jnp.bfloat16)

    def part_copy(way, step, o):
        half = cols // 2
        at = pl.ds(pl.multiple_of(ring.owner(way, step) * cols + way * half, half), half)
        return pltpu.make_async_remote_copy(
            src_ref=share.at[pl.ds(pl.multiple_of(others[o] * span, span), span), at],
            dst_ref=share_in.at[o, :, at],
            send_sem=part_send.at[way, step, o],
            recv_sem=part_recv.at[way, step, o],
            device_id={"tp": others[o]},
            device_id_type=mesh_id,
        )

    def project_out(step):
        half = cols // 2
        for way in range(2):
            at = pl.ds(pl.multiple_of(ring.owner(way, step) * cols + way * half, half), half)
            share[:, at] = (
                jnp.dot(branch[...], full_conv[:, at], preferred_element_type=jnp.float32)
                + jnp.dot(attn[...], full_attn[:, at], preferred_element_type=jnp.float32)
            ).astype(jnp.bfloat16)
        for way in range(2):
            for o in range(splits - 1):
                part_copy(way, step, o).start()

    def run(phase, plan):
        for step in range(count - 1):
            items = plan[step] if step < len(plan) else ()
            pieces = len(phases[phase][0])
            for piece in range(pieces):
                for item in items[
                    piece * len(items) // pieces : (piece + 1) * len(items) // pieces
                ]:
                    item()
                ring.advance(phase, step, piece)
            if step == count - 3 and phase + 1 < len(phases):
                ring.begin(phase + 1)

    each = functools.partial

    def spread(items, steps):
        return [
            items[i * len(items) // steps : (i + 1) * len(items) // steps] for i in range(steps)
        ]

    opening = [each(norm, i) for i in range(rows // 64)] + [each(table, i) for i in range(blocks)]
    run(0, spread(opening, count - 1))
    for item in local:
        item.wait()

    def send_rows():
        halos[0].start()
        halos[1].start()

    def take_rows():
        halos[0].wait_recv()
        halos[1].wait_recv()

    sides = [each(attention_side, i) for i in range(blocks)]
    sides.append(send_rows)
    sides += [each(attend, i) for i in range(1, blocks)]
    sides += [take_rows, each(attend, 0)]
    run(1, spread(sides, count - 1))
    opening = [each(conv_side, i) for i in range(blocks)] + [halos[2].start]
    middle_work = [take_halo] + [each(convolve, i) for i in range(tiles)] + [send_stats]
    early = spread(opening + middle_work, 3)
    late = [finish_conv] + [each(project_out, i) for i in range(count - 1)]
    if count > 6:
        tail_work = [late[:3], late[3:6]] + [[item] for item in late[6:]]
        run(2, early + tail_work)
        project_out(count - 1)
    else:
        run(2, early)
        for item in late:
            item()
        project_out(count - 1)
    ring.drain()
    for halo in halos:
        halo.wait_send()
    for o in range(splits - 1):
        stat_copy(o).wait_send()
    for step in range(count):
        for way in range(2):
            for o in range(splits - 1):
                part_copy(way, step, o).wait()
    total = share[pl.ds(pl.multiple_of(rank * span, span), span), :].astype(jnp.float32)
    for o in range(splits - 1):
        total = total + share_in[o].astype(jnp.float32)
    mixed_out[...] = total.astype(jnp.bfloat16)


def fits(count, splits, tokens, w_query, w_key, out_conv):
    rows, width = tokens.shape
    depth, wide = w_query.shape
    if depth % 128 or wide % 512 or out_conv.shape[1] % 256 or rows % (128 * splits):
        return False
    if w_key.shape[1] != 2 * HEAD_DIM or wide != 4 * w_key.shape[1] or rows > 64 * 128:
        return False
    return count % 2 == 0 and 3 < count <= 16 and splits > 1


def one_kernel(
    tokens,
    norm_gain,
    w_conv_value,
    w_conv_gate,
    w_query,
    w_key,
    w_value,
    conv_taps,
    ln_gain,
    sinks,
    out_conv,
    out_attn,
):
    count, splits = lax.axis_size("sp"), lax.axis_size("tp")
    rows, width = tokens.shape
    wide, narrow = w_query.shape[1], w_key.shape[1]
    long = out_conv.shape[0]
    full_cols = count * out_conv.shape[1]
    tiles = wide // 128
    edge = 32
    span = rows // splits
    vmem = pl.BlockSpec(memory_space=pltpu.VMEM)
    low = lambda *dims: pltpu.VMEM(dims, jnp.bfloat16)
    high = lambda *dims: pltpu.VMEM(dims, jnp.float32)
    dma = lambda *dims: pltpu.SemaphoreType.DMA(dims)
    return pl.pallas_call(
        functools.partial(layer_kernel, count, splits),
        out_shape=(
            jax.ShapeDtypeStruct((span, full_cols), jnp.bfloat16),
            jax.ShapeDtypeStruct((wide // HEAD_DIM, rows), jnp.float32),
        ),
        in_specs=[vmem] * 9 + [pl.BlockSpec(memory_space=pltpu.SMEM)] + [vmem] * 2,
        out_specs=(vmem,) * 2,
        scratch_shapes=[
            low(rows, width),
            low(width, wide),
            low(width, wide),
            low(width, wide),
            low(width, narrow),
            low(width, narrow),
            low(long, full_cols),
            low(long, full_cols),
            low(rows, wide),
            low(rows + WINDOW, narrow),
            low(rows + WINDOW, narrow),
            low(rows, wide),
            high(tiles, rows + edge, 128),
            low(edge, wide),
            low(edge, wide),
            high(tiles, rows, 128),
            high(rows, 128),
            high(rows, 128),
            high(128, 128),
            high(splits - 1, 128, 128),
            low(rows, wide),
            low(rows, full_cols),
            low(splits - 1, span, full_cols),
            dma(2, 7, count - 1),
            dma(2, 7, count - 1),
            dma(7),
            dma(3),
            dma(3),
            dma(splits - 1),
            dma(splits - 1),
            dma(2, count, splits - 1),
            dma(2, count, splits - 1),
            high(rows, 128),
            high(rows, 128),
        ],
        compiler_params=pltpu.CompilerParams(collective_id=0, has_side_effects=True),
        name="layer",
    )(
        tokens,
        norm_gain,
        w_conv_value,
        w_conv_gate,
        w_query,
        w_key,
        w_value,
        conv_taps,
        ln_gain.reshape(1, -1),
        sinks,
        out_conv,
        out_attn,
    )


def plain(tokens, norm_gain, w_conv_value, w_conv_gate, w_query, w_key, w_value, out_conv, out_attn):
    as_float = tokens.astype(jnp.float32)
    normed = (
        as_float
        * lax.rsqrt(jnp.mean(as_float * as_float, axis=-1, keepdims=True) + NORM_EPS)
        * norm_gain.astype(jnp.float32)
    ).astype(jnp.bfloat16)
    pieces = (
        lax.all_gather(w_conv_value, "sp", axis=0, tiled=True),
        lax.all_gather(w_conv_gate, "sp", axis=0, tiled=True),
        lax.all_gather(w_query, "sp", axis=0, tiled=True),
        lax.all_gather(w_key, "sp", axis=0, tiled=True),
        lax.all_gather(w_value, "sp", axis=0, tiled=True),
    )
    projected = tuple(
        (jnp.dot(normed, piece, preferred_element_type=jnp.float32) for piece in pieces)
    )
    conv_value, conv_gate, query_raw, key_raw, value_rows = [
        item.astype(jnp.bfloat16) for item in projected
    ]
    glu = (conv_value.astype(jnp.float32) * jax.nn.sigmoid(conv_gate.astype(jnp.float32))).astype(
        jnp.bfloat16
    )
    cols_conv, cols_attn = (
        lax.all_gather(out_conv, "sp", axis=1, tiled=True),
        lax.all_gather(out_attn, "sp", axis=1, tiled=True),
    )
    return glu, query_raw, key_raw, value_rows, cols_conv, cols_attn


def shards(
    tokens,
    norm_gain,
    w_conv_value,
    w_conv_gate,
    w_query,
    w_key,
    w_value,
    conv_taps,
    ln_gain,
    sinks,
    out_conv,
    out_attn,
):
    row_count = tokens.shape[0]
    if fits(lax.axis_size("sp"), lax.axis_size("tp"), tokens, w_query, w_key, out_conv):
        return one_kernel(
            tokens,
            norm_gain,
            w_conv_value,
            w_conv_gate,
            w_query,
            w_key,
            w_value,
            conv_taps,
            ln_gain,
            sinks,
            out_conv,
            out_attn,
        )
    glu, query_raw, key_raw, value_rows, cols_conv, cols_attn = plain(
        tokens, norm_gain, w_conv_value, w_conv_gate, w_query, w_key, w_value, out_conv, out_attn
    )
    offset = lax.axis_index("sp") * row_count
    positions = offset + jnp.arange(row_count, dtype=jnp.int32)
    query_heads = query_raw.shape[1] // HEAD_DIM
    key_heads = key_raw.shape[1] // HEAD_DIM
    query = rotate(query_raw.reshape(row_count, query_heads, HEAD_DIM), positions).astype(
        jnp.bfloat16
    )
    key = rotate(key_raw.reshape(row_count, key_heads, HEAD_DIM), positions).astype(jnp.bfloat16)
    reach = conv_taps.shape[0] - 1
    key_tail = key[row_count - WINDOW :]
    value_tail = value_rows.reshape(row_count, key_heads, HEAD_DIM)[row_count - WINDOW :]
    glu_tail = glu[row_count - reach :]
    glu_before = shifted(glu_tail, "sp", 1)
    key_before, value_before = shifted((key_tail, value_tail), "sp", 1)
    extended = jnp.concatenate([glu_before, glu], axis=0).astype(jnp.float32)
    conv_out = jnp.zeros((row_count, glu.shape[1]), jnp.float32)
    for tap in range(reach + 1):
        conv_out = conv_out + conv_taps[tap][None, :] * extended[tap : tap + row_count]
    sum_first = jnp.sum(conv_out, axis=-1)
    sum_second = jnp.sum(conv_out * conv_out, axis=-1)
    total_first, total_second = lax.psum((sum_first, sum_second), "tp")
    mean = (total_first / CONV_CH)[:, None]
    var = (total_second / CONV_CH)[:, None] - mean * mean
    conv_branch = jax.nn.silu(
        (conv_out - mean) * lax.rsqrt(var + CHANNEL_EPS) * ln_gain[None, :]
    ).astype(jnp.bfloat16)
    group = HEADS // KV_HEADS
    blocks = row_count // WINDOW
    q_blocks = query.reshape(blocks, WINDOW, key_heads, group, HEAD_DIM)
    key_blocks = jnp.concatenate([key_before, key], axis=0).reshape(
        blocks + 1, WINDOW, key_heads, HEAD_DIM
    )
    value_all = jnp.concatenate(
        [value_before, value_rows.reshape(row_count, key_heads, HEAD_DIM)], axis=0
    )
    value_blocks = value_all.reshape(blocks + 1, WINDOW, key_heads, HEAD_DIM)
    key_window = jnp.concatenate([key_blocks[:-1], key_blocks[1:]], axis=1)
    value_window = jnp.concatenate([value_blocks[:-1], value_blocks[1:]], axis=1)
    scores = jnp.einsum(
        "nqhgd,nkhd->nhgqk", q_blocks, key_window, preferred_element_type=jnp.float32
    ) * HEAD_DIM ** (-0.5)
    query_index = jnp.arange(WINDOW)[:, None] + WINDOW
    key_index = jnp.arange(2 * WINDOW)[None, :]
    band = (key_index <= query_index) & (query_index - key_index < WINDOW)
    block_index = jnp.arange(blocks)[:, None, None]
    allowed = band[None] & (offset + block_index * WINDOW + key_index[None] - WINDOW >= 0)
    allowed = allowed[:, None, None]
    totals = jnp.sum(jnp.where(allowed, jnp.exp(scores), 0.0), axis=-1)
    totals = totals + jnp.exp(sinks).reshape(1, key_heads, group, 1)
    log_total = jnp.log(totals)
    weights = jnp.where(allowed, jnp.exp(scores - log_total[..., None]), 0.0).astype(jnp.bfloat16)
    attended = jnp.einsum(
        "nhgqk,nkhd->nqhgd", weights, value_window, preferred_element_type=jnp.float32
    )
    attn_branch = attended.astype(jnp.bfloat16).reshape(row_count, query_heads * HEAD_DIM)
    log_sums = log_total.transpose(1, 2, 0, 3).reshape(query_heads, row_count)
    mixed = lax.psum_scatter(
        (
            jnp.dot(conv_branch, cols_conv, preferred_element_type=jnp.float32)
            + jnp.dot(attn_branch, cols_attn, preferred_element_type=jnp.float32)
        ).astype(jnp.bfloat16),
        "tp",
        scatter_dimension=0,
        tiled=True,
    )
    return (mixed, log_sums)


def solution(mesh):
    in_specs = (
        P("sp", None),
        P(),
        P("sp", "tp"),
        P("sp", "tp"),
        P("sp", "tp"),
        P("sp", "tp"),
        P("sp", "tp"),
        P(None, "tp"),
        P("tp"),
        P("tp"),
        P("tp", "sp"),
        P("tp", "sp"),
    )
    out_specs = (P(("sp", "tp"), None), P("tp", "sp"))
    return jax.shard_map(shards, mesh=mesh, in_specs=in_specs, out_specs=out_specs, check_vma=False)
```
